32 devices in a mesh: sp: 8 (over z, x), tp: 4 (over y, core).
Axes of the slice: x: 2, y: 2, z: 4, core: 2. Of those that a mesh axis runs over, the one named last changes fastest.
Arguments:
- result_cotangent_values: bfloat16 [1024, 2048], P('sp'), may hold values from -6 to 6
- specialist_entry_vectors: bfloat16 [1024, 2048], P('sp'), may hold values from -6 to 6
- chosen_specialists: int32 [1024, 2], P('sp'), may hold values from 0 to 3, all different within a row; in each aligned block of 128 rows (0 to 127, 128 to 255, ...) at most 128 rows name the same one
- specialist_mixing_shares: float32 [1024, 2], P('sp'), may hold values from 0.1 to 0.9
- specialist_switch_maps: bfloat16 [8, 2048, 1792], P('sp', None, 'tp'), may hold values from -0.125 to 0.125
- specialist_widen_maps: bfloat16 [8, 2048, 1792], P('sp', None, 'tp'), may hold values from -0.125 to 0.125
- specialist_shrink_maps: bfloat16 [8, 1792, 2048], P('sp', 'tp'), may hold values from -0.09375 to 0.09375
- memory_readout_map: bfloat16 [2048, 2048], P('sp', 'tp'), may hold values from -0.125 to 0.125
- memory_source_vectors: bfloat16 [1024, 2048], P('sp', 'tp'), may hold values from -6 to 6
- memory_hidden_values: bfloat16 [1024, 2048], P('sp', 'tp'), may hold values from -6 to 6
- feature_fading_speed: float32 [2048], P('tp'), may hold values from 1.6276042e-05 to 0.009
- extra_log_fading: float32 [1024], P('sp'), may hold values from -2.8 to 0
- memory_switch_tiles: bfloat16 [8, 256, 256], P('tp'), may hold values from -0.375 to 0.375
- entry_switch_tiles: bfloat16 [8, 256, 256], P('tp'), may hold values from -0.375 to 0.375
Outputs:
- gate_proj_grad: bfloat16 [8, 2048, 1792], P('sp', None, 'tp')
- up_proj_grad: bfloat16 [8, 2048, 1792], P('sp', None, 'tp')
- down_proj_grad: bfloat16 [8, 1792, 2048], P('sp', 'tp')
- out_proj_grad: float32 [2048, 2048], P('sp', 'tp')
- lru_input_grad: float32 [1024, 2048], P('sp', 'tp')
The draws below stay inside these ranges and needn't reach their ends.
Inputs may be any that keep to these rules, and one draw needn't show every extreme that they name: `chosen_specialists`: each token names two different experts; among the 128 tokens of one device no expert is named more than 128 times, a bound that some block reaches on some device.
All inputs are finite; a program needn't handle non-finite values.
Results may differ from the reference program's by a relative error of at most 0.009.
Values may be sent and summed in bfloat16 or wider, within the bound.
A program may use at most 128 MiB of HBM per device.

```python
import math
import jax
import jax.numpy as jnp
import numpy as np
from jax import lax

D = 2048
FE = 3584
BLOCKS = 8
SLICES = 2
TOPK = 2
TOK_DEV = 128
SEQ = 1024
BW = 256
EXPERTS = 4
CAPACITY = 128
FE_PART = 1792
PARTS_SIZE = 8
FE_DEV = 448
N_SP = 8
N_TP = 4


def draw_feature_fading_speed(key, part):
    pick_key, slow_key, fast_key = jax.random.split(key, 3)
    share = 0.5
    slow_mask = jax.random.uniform(pick_key, (D,), jnp.float32) < share
    slow_rate = jnp.exp(jax.random.uniform(slow_key, (D,), jnp.float32, jnp.log(0.02), jnp.log(0.25))) / SEQ
    fast_rate = jnp.exp(jax.random.uniform(fast_key, (D,), jnp.float32, jnp.log(0.005), jnp.log(0.0085)))
    return jnp.where(slow_mask, slow_rate, fast_rate)


def draw_extra_log_fading(key, part):
    where_key, size_key = jax.random.split(key)
    spots = jax.random.randint(where_key, (4,), 0, SEQ)
    keeping = jax.random.uniform(size_key, (4,), jnp.float32, 0.5, 0.8)
    hits = (jnp.arange(SEQ, dtype=jnp.int32)[:, None] == spots[None, :]).astype(jnp.float32)
    return jnp.sum(hits * jnp.log(keeping)[None, :], axis=1)


def spiked(values, key, source, target, shards_of, factor):
    def block_of(dim):
        return (jnp.arange(values.shape[dim]) // (values.shape[dim] // shards_of)).reshape((-1,) + (1,) * (values.ndim - 1 - dim))

    one_side = jax.random.permutation(key, shards_of)[block_of(target)]
    second = (block_of(target) + shards_of // 2) % shards_of
    return jnp.where((block_of(source) == one_side) | (block_of(source) == second), factor * values, values)


def level_of(stream_key, shape, cuts, low, top_value):
    def one(position, shards_of):
        heights = jax.random.uniform(jax.random.fold_in(jax.random.fold_in(stream_key, 6), position), (shards_of,), jnp.float32, low / len(cuts), top_value / len(cuts))
        return jnp.repeat(jnp.exp(heights), shape[position] // shards_of).reshape((-1,) + (1,) * (len(shape) - position - 1))

    factor_of = one(*cuts[0])
    for cut in cuts[1:]:
        factor_of = factor_of * one(*cut)
    return factor_of


def shared_out(rng, own, number, rows, count, top, reach, lean):
    order = jax.random.permutation(rng, count)
    heavy_load, ordinary = portions_of(count, rows * top, reach, lean, True), portions_of(count, rows * top, reach, lean, False)
    places = jnp.arange(count)

    def named(tallies, offset_by):
        used = int((tallies > 0).sum())
        fixed = max(1, used // 4)
        passed = fixed + (places - fixed + offset_by * (used - fixed)) % max(1, count - fixed)
        return jnp.zeros((count,), jnp.int32).at[order[jnp.where(places < fixed, places, passed)]].set(jnp.asarray(tallies, jnp.int32))

    tallies = jnp.where(number % 4 == 0, named(heavy_load, number // 4), named(ordinary, number - number // 4 - 1))
    mixed = jax.random.permutation(jax.random.fold_in(own, 3), count)
    donor, receiver = mixed[0:count // 2 * 2:2], mixed[1:count // 2 * 2:2]
    room = jnp.minimum(tallies[donor] - 1, reach - tallies[receiver]) // 2
    room = jnp.where((donor == order[0]) | (receiver == order[0]) | (tallies[receiver] == 0), 0, jnp.maximum(room, 0))
    passed = jax.random.randint(jax.random.fold_in(own, 4), (count // 2,), 0, 1 << 20) % (room + 1)
    tallies = tallies.at[donor].add(-passed).at[receiver].add(passed)
    items = jnp.searchsorted(jnp.cumsum(tallies), jnp.arange(rows * top), side="right").astype(jnp.int32)
    listing = items.reshape(top, rows).T
    listing = listing[jax.random.permutation(jax.random.fold_in(own, 1), rows)]
    offset_by = jax.random.randint(jax.random.fold_in(own, 2), (rows, 1), 0, top)
    return jnp.take_along_axis(listing, (jnp.arange(top)[None, :] + offset_by) % top, axis=1)


def portions_of(count, total, most, slope, full):
    weights = [(1 << 20) // math.isqrt(rank ** slope) + 1 for rank in range(1, count + 1)]
    largest = most if full else min(most, max(-(-total // count), total * weights[0] // sum(weights)))
    least = 1 if total - largest >= count - 1 else 0
    given, spare = [largest] + [least] * (count - 1), total - largest - least * (count - 1)
    while spare > 0:
        free = [i for i in range(1, count) if given[i] < largest] or [i for i in range(1, count) if given[i] < most]
        pool, remaining = sum([weights[i] for i in free]), spare
        for i in free:
            more = min(most - given[i], max(1, remaining * weights[i] // pool), spare)
            given[i] = given[i] + more
            spare = spare - more
    return np.array(given)


def scatter_about(key, dims, width, limit, pieces=(), held_as=jnp.bfloat16):
    result = jax.random.normal(key, dims, jnp.float32) * width
    if len(pieces) > 0:
        result = level_of(key, dims, pieces, -0.22, 0.18) * result
    return jnp.clip(result, min=-limit, max=limit).astype(held_as)


def bell_draw_with(key, extent, deviation, bound, shards, heavy, held_as=jnp.bfloat16):
    entries = deviation * jax.random.normal(key, extent, jnp.float32)
    if shards:
        entries = entries * level_of(key, extent, shards, -0.22, 0.18)
    return jnp.clip(spiked(entries, jax.random.fold_in(key, 3), *heavy), -bound, bound).astype(held_as)


def setup_inputs(seed: int = 0) -> dict:
    keys = jax.random.split(jax.random.key(seed), 15)
    result_cotangent_values = bell_draw_with(keys[0], (SEQ, D), 1.0, 6.0, ((0, 8),), (0, 1, 8, 2.0))
    specialist_entry_vectors = scatter_about(keys[1], (SEQ, D), 1.0, 6.0, ((0, 8),))
    chosen_specialists_keys = jax.random.split(jax.random.fold_in(keys[2], 1), SEQ // TOK_DEV)
    chosen_specialists_turns = jax.random.permutation(jax.random.fold_in(keys[2], 3), SEQ // TOK_DEV)
    chosen_specialists = jax.vmap(lambda own, number: shared_out(jax.random.fold_in(keys[2], 2), own, number, TOK_DEV, EXPERTS, TOPK, CAPACITY, 1))(chosen_specialists_keys, chosen_specialists_turns).reshape((SEQ, TOPK))
    specialist_mixing_shares = jnp.clip(0.1 + 0.79999997 * jax.random.uniform(keys[3], (SEQ, TOPK), jnp.float32) ** level_of(keys[3], (SEQ, TOPK), ((0, 8),), -0.2, 0.2), 0.1, 0.9)
    specialist_switch_maps = scatter_about(keys[4], (EXPERTS * SLICES, D, FE_PART), D ** -0.5, 0.125, ((0, 8), (2, 4)))
    specialist_widen_maps = scatter_about(keys[5], (EXPERTS * SLICES, D, FE_PART), D ** -0.5, 0.125, ((0, 8), (2, 4)))
    specialist_shrink_maps = scatter_about(keys[6], (EXPERTS * SLICES, FE_PART, D), FE ** -0.5, 0.09375, ((0, 8), (1, 4)))
    memory_readout_map = scatter_about(keys[7], (D, D), D ** -0.5, 0.125, ((0, 8), (1, 4)))
    memory_source_vectors = scatter_about(keys[8], (SEQ, D), 1.0, 6.0, ((0, 8), (1, 4)))
    memory_hidden_values = scatter_about(keys[9], (SEQ, D), 1.0, 6.0, ((0, 8), (1, 4)))
    feature_fading_speed = draw_feature_fading_speed(jax.random.fold_in(keys[14], 71), 0)
    extra_log_fading = draw_extra_log_fading(jax.random.fold_in(keys[14], 71), 0)
    memory_switch_tiles = scatter_about(keys[12], (BLOCKS, BW, BW), BW ** -0.5, 0.375, ((0, 4),))
    entry_switch_tiles = scatter_about(keys[13], (BLOCKS, BW, BW), BW ** -0.5, 0.375, ((0, 4),))
    return dict(result_cotangent_values=result_cotangent_values, specialist_entry_vectors=specialist_entry_vectors, chosen_specialists=chosen_specialists, specialist_mixing_shares=specialist_mixing_shares, specialist_switch_maps=specialist_switch_maps, specialist_widen_maps=specialist_widen_maps, specialist_shrink_maps=specialist_shrink_maps, memory_readout_map=memory_readout_map, memory_source_vectors=memory_source_vectors, memory_hidden_values=memory_hidden_values, feature_fading_speed=feature_fading_speed, extra_log_fading=extra_log_fading, memory_switch_tiles=memory_switch_tiles, entry_switch_tiles=entry_switch_tiles)


def silu_slope(value):
    sig_value = jax.nn.sigmoid(value)
    return sig_value * (1.0 + value * (1.0 - sig_value))

def compose(upper_map, lower_map):
    return (lower_map[0] * upper_map[0], lower_map[1] + lower_map[0] * upper_map[1])

def slot_index(chosen_specialists):
    flat_expert = chosen_specialists.reshape(N_SP, TOPK * TOK_DEV)
    onehot = (flat_expert[:, :, None] == jnp.arange(EXPERTS, dtype=jnp.int32)[None, None, :]).astype(jnp.int32)
    slot_rank = lax.optimization_barrier(jnp.sum((jnp.cumsum(onehot, axis=1) - 1) * onehot, axis=2))
    source = jnp.arange(N_SP, dtype=jnp.int32)[:, None]
    index = (flat_expert * N_SP + source) * CAPACITY + slot_rank
    return index.reshape(-1).astype(jnp.int32)

def expert_pass(args):
    inputs, grads_in, gate_weight, up_weight, down_weight = args
    x_val = inputs.astype(jnp.float32)
    y_val = grads_in.astype(jnp.float32)
    gate_full = gate_weight.astype(jnp.float32)
    up_full = up_weight.astype(jnp.float32)
    down_full = down_weight.astype(jnp.float32)
    gate_value = jnp.einsum('rd,pdf->prf', x_val, gate_full)
    up_value = jnp.einsum('rd,pdf->prf', x_val, up_full)
    active = jax.nn.silu(gate_value)
    hidden = lax.optimization_barrier((active * up_value).astype(jnp.bfloat16)).astype(jnp.float32)
    down_grad = jnp.einsum('prf,rd->pfd', hidden, y_val).astype(jnp.bfloat16)
    hidden_grad = jnp.einsum('rd,pfd->prf', y_val, down_full)
    gate_grad = lax.optimization_barrier((hidden_grad * up_value * silu_slope(gate_value)).astype(jnp.bfloat16)).astype(jnp.float32)
    up_grad = lax.optimization_barrier((hidden_grad * active).astype(jnp.bfloat16)).astype(jnp.float32)
    gate_weight_grad = jnp.einsum('rd,prf->pdf', x_val, gate_grad).astype(jnp.bfloat16)
    up_weight_grad = jnp.einsum('rd,prf->pdf', x_val, up_grad).astype(jnp.bfloat16)
    token_part = jnp.einsum('prf,pdf->prd', gate_grad, gate_full) + jnp.einsum('prf,pdf->prd', up_grad, up_full)
    rounded = lax.optimization_barrier(token_part.astype(jnp.bfloat16)).astype(jnp.float32)
    return (gate_weight_grad, up_weight_grad, down_grad, lax.optimization_barrier(jnp.sum(rounded, axis=0)))

def reference(result_cotangent_values, specialist_entry_vectors, chosen_specialists, specialist_mixing_shares, specialist_switch_maps, specialist_widen_maps, specialist_shrink_maps, memory_readout_map, memory_source_vectors, memory_hidden_values, feature_fading_speed, extra_log_fading, memory_switch_tiles, entry_switch_tiles):
    index = slot_index(chosen_specialists)
    sent = (specialist_mixing_shares[:, :, None] * result_cotangent_values[:, None, :].astype(jnp.float32)).astype(jnp.bfloat16).reshape(SEQ * TOPK, D)
    copies = jnp.broadcast_to(specialist_entry_vectors[:, None, :], (SEQ, TOPK, D)).reshape(SEQ * TOPK, D)
    total_rows = EXPERTS * N_SP * CAPACITY
    grads_in = jnp.zeros((total_rows, D), jnp.bfloat16).at[index].set(sent).reshape(EXPERTS, N_SP * CAPACITY, D)
    inputs = jnp.zeros((total_rows, D), jnp.bfloat16).at[index].set(copies).reshape(EXPERTS, N_SP * CAPACITY, D)
    gate_parts = specialist_switch_maps.reshape(EXPERTS, SLICES, D, N_TP, FE_DEV).transpose(0, 1, 3, 2, 4).reshape(EXPERTS, PARTS_SIZE, D, FE_DEV)
    up_parts = specialist_widen_maps.reshape(EXPERTS, SLICES, D, N_TP, FE_DEV).transpose(0, 1, 3, 2, 4).reshape(EXPERTS, PARTS_SIZE, D, FE_DEV)
    down_parts = specialist_shrink_maps.reshape(EXPERTS, PARTS_SIZE, FE_DEV, D)
    gate_grads, up_grads, down_grads, partials = lax.map(expert_pass, (inputs, grads_in, gate_parts, up_parts, down_parts))
    moe_grad = jnp.take(partials.reshape(total_rows, D), index, axis=0).reshape(SEQ, TOPK, D).sum(axis=1)
    mixed_grad = (result_cotangent_values.astype(jnp.float32) + moe_grad).astype(jnp.bfloat16)
    upstream = jnp.dot(mixed_grad, memory_readout_map, preferred_element_type=jnp.float32)
    xin = memory_source_vectors.astype(jnp.float32)
    blocks_in = xin.reshape(SEQ, BLOCKS, BW)
    rec_full = memory_switch_tiles.astype(jnp.float32)
    in_full = entry_switch_tiles.astype(jnp.float32)
    memory_switch_fraction = jax.nn.sigmoid(jnp.einsum('tnc,ncd->tnd', blocks_in, rec_full).reshape(SEQ, D))
    inp_open = jax.nn.sigmoid(jnp.einsum('tnc,ncd->tnd', blocks_in, in_full).reshape(SEQ, D))
    log_fading_factor = -8.0 * memory_switch_fraction * feature_fading_speed[None, :] + extra_log_fading[:, None]
    decay_mult = jnp.exp(log_fading_factor)
    spare_room = -jnp.expm1(2.0 * log_fading_factor)
    in_scale = jnp.sqrt(jnp.maximum(spare_room, 0.01))
    drive = in_scale * inp_open * xin
    coeff = jnp.concatenate([decay_mult[1:], jnp.ones((1, D), jnp.float32)], axis=0)
    _, dstate = lax.associative_scan(compose, (coeff, upstream), reverse=True, axis=0)
    scale_slope = jnp.where(spare_room > 0.01, -decay_mult * decay_mult / in_scale, 0.0)
    log_grad = dstate * (memory_hidden_values.astype(jnp.float32) - drive + scale_slope * inp_open * xin)
    grad_rec = lax.optimization_barrier((log_grad * (-8.0 * feature_fading_speed[None, :]) * memory_switch_fraction * (1.0 - memory_switch_fraction)).astype(jnp.bfloat16)).astype(jnp.float32)
    grad_in = lax.optimization_barrier((dstate * in_scale * xin * inp_open * (1.0 - inp_open)).astype(jnp.bfloat16)).astype(jnp.float32)
    back_rec = jnp.einsum('tnd,ncd->tnc', grad_rec.reshape(SEQ, BLOCKS, BW), rec_full).reshape(SEQ, D)
    back_in = jnp.einsum('tnd,ncd->tnc', grad_in.reshape(SEQ, BLOCKS, BW), in_full).reshape(SEQ, D)
    lru_input_grad = dstate * in_scale * inp_open + back_rec + back_in
    out_proj_grad = jnp.dot(mixed_grad.T, memory_hidden_values, preferred_element_type=jnp.float32)
    gate_proj_grad = gate_grads.reshape(EXPERTS, SLICES, N_TP, D, FE_DEV).transpose(0, 1, 3, 2, 4).reshape(EXPERTS * SLICES, D, N_TP * FE_DEV)
    up_proj_grad = up_grads.reshape(EXPERTS, SLICES, N_TP, D, FE_DEV).transpose(0, 1, 3, 2, 4).reshape(EXPERTS * SLICES, D, N_TP * FE_DEV)
    down_proj_grad = down_grads.reshape(EXPERTS * SLICES, N_TP * FE_DEV, D)
    return (gate_proj_grad, up_proj_grad, down_proj_grad, out_proj_grad, lru_input_grad)
```

```python
import functools

import jax
import jax.numpy as jnp
from jax import lax
from jax.experimental import pallas as pl
from jax.experimental.pallas import tpu as pltpu
from jax.sharding import PartitionSpec as P

SLICES = 2


def prefix(part, axis, combine, identity):
    count = lax.axis_size(axis)
    place = lax.axis_index(axis)
    ahead = count - 1 - place
    gathered = jax.tree.map(lambda a: lax.all_gather(a, axis), part)
    state = jax.tree.map(lambda a, e: jnp.zeros_like(a) + jnp.asarray(e, a.dtype), part, identity)

    def one(turn, state):
        source = count - 1 - turn
        return combine(
            state, jax.tree.map(lambda a: lax.dynamic_index_in_dim(a, source, 0, False), gathered)
        )

    return lax.fori_loop(0, ahead, one, state)


def silu_slope(value):
    sig_value = jax.nn.sigmoid(value)
    return sig_value * (1.0 + value * (1.0 - sig_value))


def compose(upper_map, lower_map):
    return (lower_map[0] * upper_map[0], lower_map[1] + lower_map[0] * upper_map[1])


def chain_join(higher_map, lower_map):
    return (lower_map[0] * higher_map[0], lower_map[1] + lower_map[0] * higher_map[1])


def expert_backward(inputs, grads_in, gate_weight, up_weight, down_weight):
    gate_value = jnp.dot(inputs, gate_weight, preferred_element_type=jnp.float32)
    up_value = jnp.dot(inputs, up_weight, preferred_element_type=jnp.float32)
    active = jax.nn.silu(gate_value)
    hidden = (active * up_value).astype(jnp.bfloat16)
    down_grad = jnp.einsum(
        "rf,rd->fd", hidden, grads_in, preferred_element_type=jnp.float32
    ).astype(jnp.bfloat16)
    hidden_grad = jnp.einsum("rd,fd->rf", grads_in, down_weight, preferred_element_type=jnp.float32)
    gate_grad = (hidden_grad * up_value * silu_slope(gate_value)).astype(jnp.bfloat16)
    up_grad = (hidden_grad * active).astype(jnp.bfloat16)
    gate_weight_grad = jnp.einsum(
        "rd,rf->df", inputs, gate_grad, preferred_element_type=jnp.float32
    ).astype(jnp.bfloat16)
    up_weight_grad = jnp.einsum(
        "rd,rf->df", inputs, up_grad, preferred_element_type=jnp.float32
    ).astype(jnp.bfloat16)
    token_part = jnp.einsum("rf,df->rd", gate_grad, gate_weight, preferred_element_type=jnp.float32)
    token_part = token_part + jnp.einsum(
        "rf,df->rd", up_grad, up_weight, preferred_element_type=jnp.float32
    )
    return (gate_weight_grad, up_weight_grad, down_grad, token_part)


def collect(returned, targets, route_count):
    gathered = jnp.take(returned, targets[0], axis=0).astype(jnp.float32)
    for target in targets[1:]:
        gathered = gathered + jnp.take(returned, target, axis=0).astype(jnp.float32)
    return gathered.reshape(-1, route_count, gathered.shape[-1]).sum(axis=1)


def fill_slots(values, targets, slot_rows):
    buffer = jnp.zeros((slot_rows, values.shape[1]), jnp.bfloat16)
    for target in targets:
        buffer = buffer.at[target].set(values)
    return buffer


MESH_ID = pl.DeviceIdType.MESH


def greet(peers):
    barrier = pltpu.get_barrier_semaphore()
    for peer in peers:
        pl.semaphore_signal(barrier, inc=1, device_id=peer, device_id_type=MESH_ID)
    pl.semaphore_wait(barrier, len(peers))


def remote(src, dst, send, recv, peer):
    return pltpu.make_async_remote_copy(
        src_ref=src, dst_ref=dst, send_sem=send, recv_sem=recv, device_id=peer, device_id_type=MESH_ID
    )


def places(sp_count):
    me = lax.axis_index("sp")
    tp = lax.axis_index("tp")
    side, core = tp // 2, tp % 2
    peers = [(lax.rem(me + k, sp_count), tp) for k in range(sp_count)]
    sources = [lax.rem(me + sp_count - k, sp_count) for k in range(sp_count)]
    sibling = (me, side * 2 + (1 - core))
    across = (me, (1 - side) * 2 + core)
    return me, side, core, peers, sources, sibling, across


NN = (((1,), (0,)), ((), ()))
NT = (((1,), (1,)), ((), ()))
TN = (((0,), (0,)), ((), ()))


def mm(a, b, dims):
    return lax.dot_general(a, b, dims, preferred_element_type=jnp.float32)


def f32(a):
    return a.astype(jnp.float32)


def b16(a):
    return a.astype(jnp.bfloat16)


def mega_kernel(
    sp_count,
    x_ref, g_ref, ch_ref, mix_ref, r_ref, src_ref, h_ref, fade_ref, extra_ref, mt_ref, et_ref,
    wg_any, wu_any, wd_any,
    gw_any, uw_any, dw_any, outp_ref, lru_ref,
    X, Y, sbuf, wg, wu, wd, hid, dg, du, pa, sib, s1, ygot, s2, xgot, s3, s30, zgot,
    gx, M4, Rd, H, MC, gwv, uwv, dwv, ubuf, ugot, Uf, coef, pm, blk, got,
    ssem, rsem, lsem,
):
    me, side, core, peers, sources, sibling, across = places(sp_count)
    tp = lax.axis_index("tp")
    rows, feats = x_ref.shape
    half, quarter, eighth = feats // 2, feats // 4, feats // 8
    passed = 3 * half // 8
    direct = half - passed
    depth = sp_count // 2
    pair = 2 * rows
    z, x = me // 2, me % 2
    partner = (z * 2 + 1 - x, tp)
    plane = [lax.rem(z + k, depth) for k in range(depth)]
    line = [lax.rem(z + depth - k, depth) for k in range(depth)]
    along = [(plane[k] * 2 + x, tp) for k in range(depth)]
    behind = [(line[k] * 2 + x, tp) for k in range(depth)]
    first = pl.multiple_of(core * half + side * passed, 128)
    onward = pl.multiple_of(core * half + side * direct, 128)
    back = pl.multiple_of(core * half + (1 - side) * direct, 128)
    mine = pl.ds(pl.multiple_of(core * half, half), half)
    theirs = pl.ds(pl.multiple_of((1 - core) * half, half), half)
    own_q = pl.ds(pl.multiple_of(side * quarter, quarter), quarter)
    other_q = pl.ds(pl.multiple_of((1 - side) * quarter, quarter), quarter)
    own_e = pl.ds(pl.multiple_of(x * eighth, eighth), eighth)
    other_e = pl.ds(pl.multiple_of((1 - x) * eighth, eighth), eighth)
    own_rows = pl.ds(pl.multiple_of(x * rows, rows), rows)
    other_rows = pl.ds(pl.multiple_of((1 - x) * rows, rows), rows)
    spot = core * 2 + side
    count = [0]
    waiting = []

    def send(src, dst, peer):
        n = count[0]
        count[0] += 1
        cp = remote(src, dst, ssem.at[n], rsem.at[n], peer)
        cp.start()
        waiting.append(cp)
        return cp

    def at(ref, who, col, width):
        return ref.at[pl.ds(pl.multiple_of(who * rows, rows), rows), pl.ds(col, width)]

    def block(ref, who):
        return pl.ds(pl.multiple_of(who * rows, rows), rows)

    local = []
    for n, (src, dst) in enumerate(((wg_any, wg), (wu_any, wu), (wd_any, wd))):
        cp = pltpu.make_async_copy(src, dst, lsem.at[n])
        cp.start()
        local.append(cp)

    barrier = pltpu.get_barrier_semaphore()
    friends = peers[1:] + [sibling, across]
    for friend in friends:
        pl.semaphore_signal(barrier, inc=1, device_id=friend, device_id_type=MESH_ID)

    chosen, mix = ch_ref[...], mix_ref[...]

    def share(expert):
        return jnp.sum(jnp.where(chosen == expert, mix, 0.0), axis=1, keepdims=True)

    here_rows = block(X, me)
    X[here_rows, :] = x_ref[...]
    Y[here_rows, :] = b16(share(z) * f32(g_ref[...]))
    for k in range(1, depth):
        sbuf[k - 1] = b16(share(plane[k]) * f32(g_ref[:, pl.ds(first, direct)]))
    Rd[z] = r_ref[...]
    H[here_rows, :] = h_ref[...]
    pl.semaphore_wait(barrier, len(friends))

    zc, xc, yc, sc, tc = {}, {}, {}, {}, {}
    bufs = (X, Y)

    def send_z(a, k):
        src = x_ref.at[:, pl.ds(first, direct)] if a == 0 else sbuf.at[k - 1]
        zc[a, k] = send(src, at(bufs[a], me, first, direct), along[k])

    def send_x(a, k, who):
        src = x_ref.at[:, pl.ds(first, direct)] if (a == 0 and k == 0) else at(bufs[a], who, first, direct)
        xc[a, k] = send(src, at(bufs[a], who, first, direct), partner)

    def spread(a, who, n):
        ref = bufs[a]
        yc[a, n] = send(at(ref, who, onward, passed), at(ref, who, onward, passed), across)
        sc[a, n] = send(at(ref, who, first, direct), at(ref, who, first, direct), sibling)

    def source(n):
        return line[n] * 2 + x if n < depth else line[n - depth] * 2 + 1 - x

    def event_z(k):
        for a in range(2):
            zc[a, k].wait_recv()
            send_x(a, k, source(k))
            spread(a, source(k), k)

    def event_x(k):
        for a in range(2):
            xc[a, k].wait_recv()
            spread(a, source(depth + k), depth + k)

    def event_y(*ns):
        for n in ns:
            for a in range(2):
                yc[a, n].wait_recv()
                tc[a, n] = send(at(bufs[a], source(n), back, passed), at(bufs[a], source(n), back, passed), sibling)

    def settle(*ns):
        for n in ns:
            for a in range(2):
                sc[a, n].wait_recv()
                tc[a, n].wait_recv()

    def stage_a(k):
        at_rows = pl.ds(pl.multiple_of(line[k] * pair, pair), pair)
        xv = X[at_rows, :]
        gate = mm(xv, wg[...], NT)
        up = mm(xv, wu[...], NT)
        back_value = mm(Y[at_rows, :], wd[...], NT)
        sig = jax.nn.sigmoid(gate)
        act = gate * sig
        hid[at_rows, :] = b16(act * up)
        dg[at_rows, :] = b16(back_value * up * (sig * (1.0 + gate * (1.0 - sig))))
        du[at_rows, :] = b16(back_value * act)

    r1, r2, r3, r4 = {}, {}, {}, {}

    def stage_b(k):
        at_rows = pl.ds(pl.multiple_of(line[k] * pair, pair), pair)
        dgv, duv = dg[at_rows, :], du[at_rows, :]
        for cols in (theirs, mine):
            pa[k, :, cols] = b16(mm(dgv, wg[:, cols], NN) + mm(duv, wu[:, cols], NN))
            if cols is theirs:
                r1[k] = send(pa.at[k, :, theirs], sib.at[k], sibling)

    def fold_core(k):
        r1[k].wait_recv()
        s1[k] = b16(f32(pa[k, :, mine]) + f32(sib[k]))
        r2[k] = send(s1.at[k, :, other_q], ygot.at[k], across)

    def fold_y(k):
        r2[k].wait_recv()
        s2[k] = b16(f32(s1[k, :, own_q]) + f32(ygot[k]))
        r3[k] = send(s2.at[k, :, other_e], xgot.at[k], partner)

    def fold_x(k):
        r3[k].wait_recv()
        total = f32(s2[k, :, own_e]) + f32(xgot[k])
        if k == 0:
            s30[...] = total
        else:
            s3[k] = b16(total)
            r4[k] = send(s3.at[k], zgot.at[k], behind[k])

    tile = quarter
    grads = ((dg, X, gwv, gw_any), (du, X, uwv, uw_any), (hid, Y, dwv, dw_any))

    def weight_grad(n, *tiles):
        lhs, rhs, dst, out = grads[n]
        for i in tiles:
            dst[:, i * tile:(i + 1) * tile] = b16(mm(lhs[...], rhs[:, i * tile:(i + 1) * tile], TN))
            if (i + 1) * tile == feats:
                cp = pltpu.make_async_copy(dst, out, lsem.at[3 + n])
                cp.start()
                local.append(cp)

    for k in range(1, depth):
        send_z(0, k)
        if k == 1:
            send_x(0, 0, me)
        send_z(1, k)
        if k == 1:
            send_x(1, 0, me)

    blocks = mt_ref.shape[0]
    width = mt_ref.shape[1]
    source_value = src_ref[...]
    rec = jnp.concatenate(
        [mm(source_value[:, n * width:(n + 1) * width], mt_ref[n], NN) for n in range(blocks)], axis=1
    )
    inp = jnp.concatenate(
        [mm(source_value[:, n * width:(n + 1) * width], et_ref[n], NN) for n in range(blocks)], axis=1
    )
    rec, inp = jax.nn.sigmoid(rec), jax.nn.sigmoid(inp)
    xin = f32(source_value)
    rate = -8.0 * fade_ref[...]
    log_decay = rec * rate + extra_ref[...]
    decay = jnp.exp(log_decay)
    spare = 1.0 - jnp.exp(2.0 * log_decay)
    in_scale = jnp.sqrt(jnp.maximum(spare, 0.01))
    slope = jnp.where(spare > 0.01, -decay * decay / in_scale, 0.0)
    c4 = in_scale * inp
    coef[0] = (f32(h_ref[...]) - c4 * xin + slope * inp * xin) * rate * rec * (1.0 - rec)
    coef[1] = in_scale * xin * inp * (1.0 - inp)
    coef[2] = c4
    coef[3] = decay
    row = lax.broadcasted_iota(jnp.int32, decay.shape, 0)
    prod = jnp.where(row < rows - 1, pltpu.roll(decay, rows - 1, 0), 1.0)
    step, level = 1, 0
    while step < rows:
        keep = row < rows - step
        pm[level] = jnp.where(keep, prod, 0.0)
        prod = prod * jnp.where(keep, pltpu.roll(prod, rows - step, 0), 1.0)
        step, level = step * 2, level + 1
    coef[4] = prod

    for cp in local[:3]:
        cp.wait()
    event_x(0)
    event_z(1)
    event_y(depth)
    settle(depth)
    stage_a(0)
    event_x(1)
    stage_b(0)
    event_y(1, depth + 1)
    event_z(2)
    settle(1, depth + 1)
    stage_a(1)
    fold_core(0)
    event_x(2)
    stage_b(1)
    event_y(2, depth + 2)
    event_z(3)
    readout = {k: send(r_ref, Rd.at[z], along[k]) for k in range(1, depth)}
    piece = pl.ds(pl.multiple_of(core * half + side * quarter + (1 - x) * eighth, eighth), eighth)
    raw = send(g_ref.at[:, piece], gx, partner)
    settle(2, depth + 2)
    stage_a(2)
    fold_core(1)
    event_x(3)
    stage_b(2)
    fold_y(0)
    event_y(3, depth + 3)
    settle(3, depth + 3)
    stage_a(3)
    fold_core(2)
    stage_b(3)
    fold_y(1)
    fold_x(0)
    fold_core(3)
    weight_grad(0, 0, 1)
    fold_y(2)
    fold_x(1)
    weight_grad(0, 2, 3)
    weight_grad(1, 0)
    fold_y(3)
    fold_x(2)
    weight_grad(1, 1, 2, 3)
    fold_x(3)
    saved = {k: send(h_ref, H.at[here_rows, :], along[k]) for k in range(1, depth)}
    saved_x = {0: send(h_ref, H.at[here_rows, :], partner)}
    weight_grad(2, 0, 1, 2, 3)
    raw.wait_recv()
    for k in range(1, depth):
        r4[k].wait_recv()
    cols = pl.ds(pl.multiple_of(core * half + side * quarter + x * eighth, eighth), eighth)
    for at_rows, value in ((own_rows, g_ref[:, cols]), (other_rows, gx[...])):
        total = s30[at_rows, :]
        for k in range(1, depth):
            total = total + f32(zgot[k, at_rows, :])
        M4[spot, at_rows, :] = b16(f32(value) + total)
    near = send(M4.at[spot], M4.at[spot], across)
    send_s = send(M4.at[spot], M4.at[spot], sibling)
    near.wait_recv()
    spot_y = core * 2 + 1 - side
    send_t = send(M4.at[spot_y], M4.at[spot_y], sibling)
    for k in range(1, depth):
        readout[k].wait_recv()
    send_s.wait_recv()
    send_t.wait_recv()

    def upstream(at_rows):
        return sum(mm(M4[n, at_rows, :], Rd[n], NN) for n in range(depth))

    ubuf[...] = b16(upstream(other_rows))
    cross = send(ubuf, ugot, partner)
    Uf[...] = upstream(own_rows)
    core_rows = pl.ds(pl.multiple_of(core * rows, rows), rows)

    def cell(who):
        return pl.ds(pl.multiple_of(who * pair + core * rows, rows), rows)

    moved = {k: send(M4.at[plane[k], core_rows, :], MC.at[cell(z), :], along[k]) for k in range(1, depth)}
    MC[pl.ds(pl.multiple_of(z * pair, pair), pair), :] = M4[z]
    cross.wait_recv()
    part = Uf[...] + f32(ugot[...])
    step, level = 1, 0
    while step < rows:
        part = part + pm[level] * pltpu.roll(part, rows - step, 0)
        step, level = step * 2, level + 1
    blk[0:1] = coef[3, 0:1] * coef[4, 0:1]
    blk[1:2] = coef[3, 0:1] * part[0:1]
    Uf[...] = part
    carried = {k: send(blk, got.at[me], peers[k]) for k in range(1, sp_count)}
    for k in range(1, depth):
        saved[k].wait_recv()
        at_rows = block(H, source(k))
        saved_x[k] = send(H.at[at_rows, :], H.at[at_rows, :], partner)
    spread_c = {}
    for k in range(1, depth):
        moved[k].wait_recv()
        spread_c[k] = send(MC.at[cell(line[k]), :], MC.at[cell(line[k]), :], sibling)
    for k in range(1, sp_count):
        carried[k].wait_recv()
    incoming = jnp.zeros((1, part.shape[1]), jnp.float32)
    for origin in range(sp_count - 1, 0, -1):
        value = got[origin]
        incoming = jnp.where(origin > me, value[1:2] + value[0:1] * incoming, incoming)
    dstate = Uf[...] + coef[4] * incoming
    grad_rec = b16(dstate * coef[0])
    grad_in = b16(dstate * coef[1])
    back_value = jnp.concatenate(
        [
            mm(grad_rec[:, n * width:(n + 1) * width], mt_ref[n], NT)
            + mm(grad_in[:, n * width:(n + 1) * width], et_ref[n], NT)
            for n in range(blocks)
        ],
        axis=1,
    )
    lru_ref[...] = dstate * coef[2] + back_value
    for k in range(depth):
        saved_x[k].wait_recv()
    for k in range(1, depth):
        spread_c[k].wait_recv()
    outp_ref[...] = mm(MC[...], H[...], TN)
    for cp in waiting:
        cp.wait_send()
    for cp in local[3:]:
        cp.wait()


def mega(sp_count, x, g, chosen, mix, readout, source, hidden, fade, extra, rec_tiles, in_tiles, wg, wu, wd):
    rows, feats = x.shape
    units = wg.shape[0]
    cols = readout.shape[1]
    depth = sp_count // 2
    total, pair, half, quarter, eighth = rows * sp_count, 2 * rows, feats // 2, feats // 4, feats // 8
    direct = half - 3 * half // 8
    levels = (rows - 1).bit_length()
    dma = pltpu.SemaphoreType.DMA

    def vb(*shape):
        return pltpu.VMEM(shape, jnp.bfloat16)

    def vf(*shape):
        return pltpu.VMEM(shape, jnp.float32)

    scratch = [
        vb(total, feats), vb(total, feats), vb(depth - 1, rows, direct),
        vb(units, feats), vb(units, feats), vb(units, feats),
        vb(total, units), vb(total, units), vb(total, units),
        vb(depth, pair, feats), vb(depth, pair, half), vb(depth, pair, half),
        vb(depth, pair, quarter), vb(depth, pair, quarter),
        vb(depth, pair, eighth), vb(depth, pair, eighth), vf(pair, eighth), vb(depth, pair, eighth),
        vb(rows, eighth), vb(depth, pair, eighth), vb(depth, readout.shape[0], cols),
        vb(total, cols), vb(total, eighth),
        vb(units, feats), vb(units, feats), vb(units, feats),
        vb(rows, cols), vb(rows, cols), vf(rows, cols), vf(5, rows, cols), vf(levels, rows, cols),
        vf(8, cols), vf(sp_count, 8, cols),
        dma((128,)), dma((128,)), dma((6,)),
    ]
    vmem, anywhere = pl.BlockSpec(memory_space=pltpu.VMEM), pl.BlockSpec(memory_space=pl.ANY)
    weight = jax.ShapeDtypeStruct((units, feats), jnp.bfloat16)
    return pl.pallas_call(
        functools.partial(mega_kernel, sp_count),
        out_shape=[
            weight, weight, weight,
            jax.ShapeDtypeStruct((eighth, cols), jnp.float32),
            jax.ShapeDtypeStruct((rows, cols), jnp.float32),
        ],
        in_specs=[vmem] * 11 + [anywhere] * 3,
        out_specs=[anywhere] * 3 + [vmem] * 2,
        scratch_shapes=scratch,
        compiler_params=pltpu.CompilerParams(
            collective_id=0, has_side_effects=True, vmem_limit_bytes=58 * 2 ** 20
        ),
    )(x, g, chosen, mix, readout, source, hidden, fade, extra, rec_tiles, in_tiles, wg, wu, wd)


def local(
    result_cotangent_values,
    specialist_entry_vectors,
    chosen_specialists,
    specialist_mixing_shares,
    specialist_switch_maps,
    specialist_widen_maps,
    specialist_shrink_maps,
    memory_readout_map,
    memory_source_vectors,
    memory_hidden_values,
    feature_fading_speed,
    extra_log_fading,
    memory_switch_tiles,
    entry_switch_tiles,
):
    tok_rows, feature_count = result_cotangent_values.shape
    route_count = chosen_specialists.shape[1]
    sp_count = lax.axis_size("sp")
    expert_count = sp_count // SLICES
    capacity = min(tok_rows, 4 * tok_rows // expert_count)
    slot_rows = sp_count * capacity
    flat_expert = chosen_specialists.reshape(-1)
    onehot = (flat_expert[:, None] == jnp.arange(expert_count, dtype=jnp.int32)[None, :]).astype(
        jnp.int32
    )
    slot_rank = jnp.sum((jnp.cumsum(onehot, axis=0) - 1) * onehot, axis=1)
    scaled = (
        (
            specialist_mixing_shares[:, :, None]
            * result_cotangent_values[:, None, :].astype(jnp.float32)
        )
        .astype(jnp.bfloat16)
        .reshape(-1, feature_count)
    )
    copies = jnp.broadcast_to(
        specialist_entry_vectors[:, None, :], (tok_rows, route_count, feature_count)
    ).reshape(-1, feature_count)
    targets = [
        (flat_expert * SLICES + slice_index) * capacity + slot_rank for slice_index in range(SLICES)
    ]
    share = feature_count // lax.axis_size("tp")
    first_col = lax.axis_index("tp") * share
    part_grad = lax.dynamic_slice_in_dim(scaled, first_col, share, 1)
    part_rows = lax.dynamic_slice_in_dim(copies, first_col, share, 1)
    send_grad = fill_slots(part_grad, targets, slot_rows)
    send_rows = fill_slots(part_rows, targets, slot_rows)
    got_grad, got_rows = (
        lax.all_to_all(
            send_grad.reshape(sp_count, capacity, share),
            "sp",
            split_axis=0,
            concat_axis=0,
            tiled=True,
        ),
        lax.all_to_all(
            send_rows.reshape(sp_count, capacity, share),
            "sp",
            split_axis=0,
            concat_axis=0,
            tiled=True,
        ),
    )
    recv_grad, recv_rows = (
        lax.all_gather(got_grad, "tp", axis=2, tiled=True),
        lax.all_gather(got_rows, "tp", axis=2, tiled=True),
    )
    inputs = recv_rows.reshape(slot_rows, feature_count)
    grads_in = recv_grad.reshape(slot_rows, feature_count)
    gate_weight_grad, up_weight_grad, down_grad, token_part = expert_backward(
        inputs,
        grads_in,
        specialist_switch_maps[0],
        specialist_widen_maps[0],
        specialist_shrink_maps[0],
    )
    returned = lax.all_to_all(
        token_part.astype(jnp.bfloat16).reshape(sp_count, capacity, feature_count),
        "sp",
        split_axis=0,
        concat_axis=0,
        tiled=True,
    )
    own_sum = collect(returned.reshape(slot_rows, feature_count), targets, route_count)
    moe_grad = lax.psum(own_sum.astype(jnp.bfloat16), "tp").astype(jnp.float32)
    mixed_grad = (result_cotangent_values.astype(jnp.float32) + moe_grad).astype(jnp.bfloat16)
    col_count = memory_readout_map.shape[1]
    columns = mixed_grad
    upstream = jnp.dot(
        columns,
        lax.all_gather(memory_readout_map, "sp", axis=0, tiled=True),
        preferred_element_type=jnp.float32,
    )
    blocks_here = memory_switch_tiles.shape[0]
    block_width = memory_switch_tiles.shape[1]
    blocks_in = memory_source_vectors.reshape(tok_rows, blocks_here, block_width)
    memory_switch_fraction = jax.nn.sigmoid(
        jnp.einsum(
            "tnc,ncd->tnd", blocks_in, memory_switch_tiles, preferred_element_type=jnp.float32
        ).reshape(tok_rows, col_count)
    )
    inp_open = jax.nn.sigmoid(
        jnp.einsum(
            "tnc,ncd->tnd", blocks_in, entry_switch_tiles, preferred_element_type=jnp.float32
        ).reshape(tok_rows, col_count)
    )
    xin = memory_source_vectors.astype(jnp.float32)
    log_fading_factor = (
        -8.0 * memory_switch_fraction * feature_fading_speed[None, :] + extra_log_fading[:, None]
    )
    decay_mult = jnp.exp(log_fading_factor)
    spare_room = -jnp.expm1(2.0 * log_fading_factor)
    in_scale = jnp.sqrt(jnp.maximum(spare_room, 0.01))
    drive = in_scale * inp_open * xin
    coeff = jnp.concatenate([decay_mult[1:], jnp.ones((1, col_count), jnp.float32)], axis=0)
    prod_after, local_part = lax.associative_scan(compose, (coeff, upstream), reverse=True, axis=0)
    alpha_part = decay_mult[0] * local_part[0]
    beta_part = decay_mult[0] * prod_after[0]
    carried = prefix(
        (beta_part, alpha_part),
        "sp",
        chain_join,
        (jnp.ones_like(beta_part), jnp.zeros_like(alpha_part)),
    )
    incoming = carried[1]
    dstate = local_part + prod_after * incoming[None, :]
    scale_slope = jnp.where(spare_room > 0.01, -decay_mult * decay_mult / in_scale, 0.0)
    log_grad = dstate * (
        memory_hidden_values.astype(jnp.float32) - drive + scale_slope * inp_open * xin
    )
    grad_rec = (
        log_grad
        * (-8.0 * feature_fading_speed[None, :])
        * memory_switch_fraction
        * (1.0 - memory_switch_fraction)
    ).astype(jnp.bfloat16)
    grad_in = (dstate * in_scale * xin * inp_open * (1.0 - inp_open)).astype(jnp.bfloat16)
    back_rec = jnp.einsum(
        "tnd,ncd->tnc",
        grad_rec.reshape(tok_rows, blocks_here, block_width),
        memory_switch_tiles,
        preferred_element_type=jnp.float32,
    )
    back_in = jnp.einsum(
        "tnd,ncd->tnc",
        grad_in.reshape(tok_rows, blocks_here, block_width),
        entry_switch_tiles,
        preferred_element_type=jnp.float32,
    )
    lru_input_grad = (
        dstate * in_scale * inp_open
        + back_rec.reshape(tok_rows, col_count)
        + back_in.reshape(tok_rows, col_count)
    )
    columns = mixed_grad
    out_proj_grad = lax.psum_scatter(
        jnp.einsum("tr,tc->rc", columns, memory_hidden_values, preferred_element_type=jnp.float32),
        "sp",
        scatter_dimension=0,
        tiled=True,
    )
    return (
        gate_weight_grad[None],
        up_weight_grad[None],
        down_grad[None],
        out_proj_grad,
        lru_input_grad,
    )


def direct(
    result_cotangent_values,
    specialist_entry_vectors,
    chosen_specialists,
    specialist_mixing_shares,
    specialist_switch_maps,
    specialist_widen_maps,
    specialist_shrink_maps,
    memory_readout_map,
    memory_source_vectors,
    memory_hidden_values,
    feature_fading_speed,
    extra_log_fading,
    memory_switch_tiles,
    entry_switch_tiles,
):
    gate_weight_grad, up_weight_grad, down_grad, out_proj_grad, lru_input_grad = mega(
        lax.axis_size("sp"),
        specialist_entry_vectors,
        result_cotangent_values,
        chosen_specialists,
        specialist_mixing_shares,
        memory_readout_map,
        memory_source_vectors,
        memory_hidden_values,
        feature_fading_speed[None, :],
        extra_log_fading[:, None],
        memory_switch_tiles,
        entry_switch_tiles,
        jnp.swapaxes(specialist_switch_maps[0], 0, 1),
        jnp.swapaxes(specialist_widen_maps[0], 0, 1),
        specialist_shrink_maps[0],
    )
    return (
        jnp.swapaxes(gate_weight_grad, 0, 1)[None],
        jnp.swapaxes(up_weight_grad, 0, 1)[None],
        down_grad[None],
        out_proj_grad,
        lru_input_grad,
    )


def solution(mesh):
    sp_count, tp_count = mesh.shape["sp"], mesh.shape["tp"]
    whole_blocks = 4 * SLICES == sp_count and tp_count == 4
    return jax.shard_map(
        direct if whole_blocks else local,
        mesh=mesh,
        in_specs=(
            P("sp", None),
            P("sp", None),
            P("sp", None),
            P("sp", None),
            P("sp", None, "tp"),
            P("sp", None, "tp"),
            P("sp", "tp", None),
            P("sp", "tp"),
            P("sp", "tp"),
            P("sp", "tp"),
            P("tp"),
            P("sp"),
            P("tp", None, None),
            P("tp", None, None),
        ),
        out_specs=(
            P("sp", None, "tp"),
            P("sp", None, "tp"),
            P("sp", "tp", None),
            P("sp", "tp"),
            P("sp", "tp"),
        ),
        check_vma=False,
    )
```
